32 devices in a mesh: fs: 8 (over z, y), tp: 4 (over x, core).
Axes of the slice: x: 2, y: 2, z: 4, core: 2. Of those that a mesh axis runs over, the one named last changes fastest.
Arguments:
- tokens: bfloat16 [8192, 2048], P('fs'), may hold values from -6 to 6
- norm_gain: float32 [2048], replicated, may hold values from 0.1 to 1.9
- gate_weight: bfloat16 [2048, 4096], P('fs', 'tp'), may hold values from -0.125 to 0.125
- up_weight: bfloat16 [2048, 4096], P('fs', 'tp'), may hold values from -0.125 to 0.125
- down_weight: bfloat16 [4096, 2048], P('tp', 'fs'), may hold values from -2 to 2
- out_gain: float32 [2048], P('tp'), may hold values from 0.1 to 1.9
Outputs:
- result: bfloat16 [8192, 2048], P('fs', 'tp')
The draws below stay inside these ranges and needn't reach their ends.
All inputs are finite; a program needn't handle non-finite values.
Results may differ from the reference program's by a relative error of at most 0.014.
Values may be sent and summed in bfloat16 or wider, within the bound.
No kernel may reach another device: no remote copies, remote signals or barrier semaphores. Data moves between devices by JAX's collectives and lax.ppermute only.
A program may use at most 64 MiB of HBM per device.

```python
import jax
import jax.numpy as jnp
from jax import lax

D = 2048
FF = 4096
TOK_DEV = 1024
TOKENS = 8192
N_FS = 8
N_TP = 4


def draw_down_weight(key, part):
    first_key, second_key = jax.random.split(jax.random.fold_in(key, 17))
    group_scales = jnp.exp(jax.random.uniform(second_key, (16,), jnp.float32, -0.9, 0.9))
    column_scale = jnp.repeat(group_scales, D // 16)
    base = jnp.clip(jax.random.normal(first_key, (FF, D), jnp.float32), -4.0, 4.0)
    values = jnp.clip(base * FF ** (-0.5) * column_scale[None, :], -2.0, 2.0)
    return values.astype(jnp.bfloat16)


def shard_levels(key, shape, cuts, low, largest):
    def one(position, parts):
        steps = jax.random.uniform(jax.random.fold_in(jax.random.fold_in(key, 6), position), (parts,), jnp.float32, low / len(cuts), largest / len(cuts))
        return jnp.repeat(jnp.exp(steps), shape[position] // parts).reshape((-1,) + (1,) * (len(shape) - position - 1))

    gain = one(*cuts[0])
    for cut in cuts[1:]:
        gain = gain * one(*cut)
    return gain


def normal_values(own_key, shape, spread, reach, cuts=(), dtype=jnp.bfloat16):
    drawn = spread * jax.random.normal(own_key, shape, jnp.float32)
    if cuts:
        drawn = drawn * shard_levels(own_key, shape, cuts, -0.22, 0.18)
    return jnp.clip(drawn, -reach, reach).astype(dtype)


def setup_inputs(seed: int = 0) -> dict:
    key_list = jax.random.split(jax.random.key(seed), 7)
    return {
        "tokens": normal_values(key_list[0], (TOKENS, D), 1.0, 6.0, ((0, 8),)),
        "norm_gain": jnp.clip(1.0 + 0.18 * jax.random.normal(key_list[1], (D,), jnp.float32), 0.1, 1.9),
        "gate_weight": normal_values(key_list[2], (D, FF), D ** -0.5, 0.125, ((0, 8), (1, 4))),
        "up_weight": normal_values(key_list[3], (D, FF), D ** -0.5, 0.125, ((0, 8), (1, 4))),
        "down_weight": draw_down_weight(jax.random.fold_in(key_list[6], 71), 0),
        "out_gain": jnp.clip(1.0 + 0.18 * jax.random.normal(key_list[5], (D,), jnp.float32), 0.1, 1.9),
    }


EPSILON = 1e-06

def reference(tokens, norm_gain, gate_weight, up_weight, down_weight, out_gain):
    width = FF // N_TP
    down_blocks = down_weight.reshape(N_TP, width, D)

    def one_block(rows):
        values = rows.astype(jnp.float32)
        normed = (values * lax.rsqrt(lax.optimization_barrier(jnp.mean(values * values, axis=1, keepdims=True)) + EPSILON) * norm_gain.astype(jnp.float32)).astype(jnp.bfloat16)
        gate_proj = jnp.dot(normed, gate_weight, preferred_element_type=jnp.float32)
        up_proj = jnp.dot(normed, up_weight, preferred_element_type=jnp.float32)
        hidden = (jax.nn.silu(gate_proj) * up_proj).astype(jnp.bfloat16)
        branch = jnp.zeros((rows.shape[0], D), jnp.float32)
        for index in range(N_TP):
            piece = jnp.dot(hidden[:, index * width:(index + 1) * width], down_blocks[index], preferred_element_type=jnp.float32).astype(jnp.bfloat16)
            branch = branch + lax.optimization_barrier(piece).astype(jnp.float32)
        mean_square = lax.optimization_barrier(jnp.mean(branch * branch, axis=1, keepdims=True))
        return (branch * lax.rsqrt(mean_square + EPSILON) * out_gain.astype(jnp.float32)).astype(jnp.bfloat16)
    blocks = tokens.reshape(N_FS, TOK_DEV, D)
    return lax.map(one_block, blocks).reshape(TOKENS, D)
```

```python
import jax
import jax.numpy as jnp
from jax import lax
from jax.sharding import PartitionSpec as P

EPSILON = 1e-06


def make_body(n_fs, n_tp):
    ring = list(range(0, n_fs, 2)) + list(range(n_fs - 1, 0, -2))
    place = [ring.index(i) for i in range(n_fs)]
    right = [(ring[i], ring[(i + 1) % n_fs]) for i in range(n_fs)]
    left = [(b, a) for a, b in right]
    far = n_fs // 2
    chips = n_tp // 2
    per_chip = n_fs // chips
    sibling = [(t, t ^ 1) for t in range(n_tp)]

    def source(i, hops):
        return ring[(place[i] - hops) % n_fs]

    def owner_chip(j):
        return j // per_chip

    def after(value, *others):
        return lax.optimization_barrier((value,) + others)[0]

    def walk(pair, gate=(), second=()):
        steps = [(0,) + tuple(pair)]
        forward = [after(x, *gate) for x in pair]
        backward = [after(x, *gate) for x in pair]
        for k in range(1, far):
            if k == 2:
                forward = [after(x, *second) for x in forward]
                backward = [after(x, *second) for x in backward]
            forward = [lax.ppermute(x, "fs", right) for x in forward]
            backward = [lax.ppermute(x, "fs", left) for x in backward]
            steps.append((k,) + tuple(forward))
            steps.append((-k,) + tuple(backward))
        steps.append((far, lax.ppermute(forward[0], "fs", right), lax.ppermute(backward[1], "fs", left)))
        return steps

    def body(tokens, norm_gain, gate_weight, up_weight, down_weight, out_gain):
        fs = lax.axis_index("fs")
        tp = lax.axis_index("tp")
        core = tp % 2
        chip = tp // 2
        rows = gate_weight.shape[0]
        cols = down_weight.shape[1]
        side = cols // 2

        def table(values):
            return jnp.asarray(values, jnp.int32)[fs]

        steps = walk((gate_weight, up_weight))

        values = tokens.astype(jnp.float32)
        normed = (
            values * lax.rsqrt(jnp.mean(values * values, axis=1, keepdims=True) + EPSILON) * norm_gain
        ).astype(jnp.bfloat16)

        gate_sum = up_sum = None
        for hops, gate_rows, up_rows in steps:
            j = table([source(i, hops) for i in range(n_fs)])
            piece = lax.dynamic_slice_in_dim(normed, j * rows, rows, axis=1)
            gate_part = jnp.dot(piece, gate_rows, preferred_element_type=jnp.float32)
            up_part = jnp.dot(piece, up_rows, preferred_element_type=jnp.float32)
            if gate_sum is None:
                gate_sum, up_sum = gate_part, up_part
            else:
                gate_sum, up_sum = lax.optimization_barrier((gate_sum + gate_part, up_sum + up_part))
        hidden = (jax.nn.silu(gate_sum) * up_sum).astype(jnp.bfloat16)
        hidden_sib = lax.ppermute(hidden, "tp", sibling)

        mine = lax.dynamic_slice_in_dim(down_weight, core * side, side, axis=1)
        give = lax.dynamic_slice_in_dim(down_weight, (1 - core) * side, side, axis=1)
        theirs = lax.ppermute(give, "tp", sibling)
        down_steps = walk((mine, theirs), gate=steps[-3][1:] + steps[-2][1:], second=(hidden_sib,))

        blocks = []
        for hops, own_rows, sib_rows in down_steps:
            partial = jnp.dot(hidden, own_rows, preferred_element_type=jnp.float32) + jnp.dot(
                hidden_sib, sib_rows, preferred_element_type=jnp.float32
            )
            sent = partial.astype(jnp.bfloat16)
            total = partial
            for shift in range(1, chips):
                pairs = []
                for i in range(n_fs):
                    to = owner_chip(source(i, hops))
                    frm = (to + shift) % chips
                    for c in range(2):
                        pairs.append((i * n_tp + frm * 2 + c, i * n_tp + to * 2 + c))
                total = total + lax.ppermute(sent, ("fs", "tp"), pairs).astype(jnp.float32)
            blocks.append(total.astype(jnp.bfloat16))
        whole = jnp.stack(blocks)

        order = [s[0] for s in down_steps]
        where = [[0] * n_fs for _ in range(n_fs)]
        for i in range(n_fs):
            for index, hops in enumerate(order):
                where[i][source(i, hops)] = index
        spots = lax.dynamic_slice_in_dim(table(where), chip * per_chip, per_chip)
        found = [lax.dynamic_index_in_dim(whole, spots[s], keepdims=False) for s in range(per_chip)]

        squares = sum(jnp.sum(jnp.square(x.astype(jnp.float32)), axis=1) for x in found)
        squares = lax.psum(squares, "tp")
        half = per_chip // 2
        low = jnp.concatenate(found[:half], axis=1)
        high = jnp.concatenate(found[half:], axis=1)
        kept = jnp.where(core == 0, low, high)
        gone = jnp.where(core == 0, high, low)
        got = lax.ppermute(gone, "tp", sibling)
        parts = []
        for s in range(half):
            a = kept[:, s * side:(s + 1) * side]
            b = got[:, s * side:(s + 1) * side]
            parts += [jnp.where(core == 0, a, b), jnp.where(core == 0, b, a)]
        own_columns = jnp.concatenate(parts, axis=1).astype(jnp.float32)
        mean_square = squares / (out_gain.shape[0] * n_tp)
        scaled = own_columns * lax.rsqrt(mean_square + EPSILON)[:, None] * out_gain[None, :]
        return scaled.astype(jnp.bfloat16)

    return body


def solution(mesh):
    return jax.shard_map(
        make_body(mesh.shape["fs"], mesh.shape["tp"]),
        mesh=mesh,
        in_specs=(P("fs", None), P(), P("fs", "tp"), P("fs", "tp"), P("tp", "fs"), P("tp")),
        out_specs=P("fs", "tp"),
        check_vma=False,
    )
```

```python
import jax
import jax.numpy as jnp
from jax import lax
from jax.sharding import PartitionSpec as P

EPSILON = 1e-06


def after(value, *others):
    return lax.optimization_barrier((value,) + others)[0]


def matmul(a, b):
    return jnp.dot(a, b, preferred_element_type=jnp.float32)


def make_body(n_fs, n_tp):
    ring = list(range(0, n_fs, 2)) + list(range(n_fs - 1, 0, -2))
    right = [(ring[i], ring[(i + 1) % n_fs]) for i in range(n_fs)]
    left = [(b, a) for a, b in right]
    far = n_fs // 2
    chips = n_tp // 2
    per_chip = n_fs // chips
    sibling = [(t, t ^ 1) for t in range(n_tp)]

    def shard_at(place):
        place = place % n_fs
        return jnp.where(place < far, 2 * place, 2 * (n_fs - 1 - place) + 1)

    def place_of(shard):
        return jnp.where(shard % 2 == 0, shard // 2, n_fs - 1 - shard // 2)

    def body(tokens, norm_gain, gate_weight, up_weight, down_weight, out_gain):
        fs = lax.axis_index("fs")
        tp = lax.axis_index("tp")
        core = tp % 2
        chip = tp // 2
        here = place_of(fs)
        rows = gate_weight.shape[0]
        side = down_weight.shape[1] // 2

        mine = lax.dynamic_slice_in_dim(down_weight, core * side, side, axis=1)
        give = lax.dynamic_slice_in_dim(down_weight, (1 - core) * side, side, axis=1)
        own = jnp.concatenate([mine, lax.ppermute(give, "tp", sibling)], axis=0)

        gates, ups = {0: gate_weight}, {0: up_weight}
        for k in range(1, far):
            if k == 2:
                gates[1] = after(gates[1], own)
            for blocks in (gates, ups):
                blocks[k] = lax.ppermute(blocks[k - 1], "fs", right)
                blocks[-k] = lax.ppermute(blocks[1 - k], "fs", left)
        gates[far] = lax.ppermute(gates[far - 1], "fs", right)
        ups[far] = lax.ppermute(ups[1 - far], "fs", left)

        values = tokens.astype(jnp.float32)
        normed = (
            values * lax.rsqrt(jnp.mean(values * values, axis=1, keepdims=True) + EPSILON) * norm_gain
        ).astype(jnp.bfloat16)
        normed = lax.optimization_barrier(normed)

        def stage(hops, sums):
            piece = jnp.concatenate(
                [
                    lax.dynamic_slice_in_dim(normed, shard_at(here - h) * rows, rows, axis=1)
                    for h in hops
                ],
                axis=1,
            )
            out = []
            for blocks, total in zip((gates, ups), sums):
                part = matmul(piece, jnp.concatenate([blocks[h] for h in hops], axis=0))
                out.append(part if total is None else total + part)
            return out

        sums = lax.optimization_barrier(stage([0], (None, None)))
        for k in range(1, far):
            sums = lax.optimization_barrier(stage([k, -k], sums))
        gate_sum, up_sum = stage([far], sums)
        hidden = (jax.nn.silu(gate_sum) * up_sum).astype(jnp.bfloat16)
        hidden_both = jnp.concatenate([hidden, lax.ppermute(hidden, "tp", sibling)], axis=1)
        hidden_both = lax.optimization_barrier(hidden_both)

        height = own.shape[0]
        own = after(own, ups[far - 1], ups[1 - far])
        downs = {0: own}
        partials = {}

        def multiply(hops):
            product = matmul(hidden_both, jnp.concatenate([downs[h] for h in hops], axis=1))
            product = product.astype(jnp.bfloat16)
            for index, h in enumerate(hops):
                partials[h % n_fs] = product[:, index * side : (index + 1) * side]
            return product

        ready = hidden_both
        for k in range(1, far):
            if k > 1:
                downs[k - 1], downs[1 - k] = lax.optimization_barrier(
                    (downs[k - 1], downs[1 - k], ready)
                )[:2]
            downs[k] = lax.ppermute(downs[k - 1], "fs", right)
            downs[-k] = lax.ppermute(downs[1 - k], "fs", left)
            if k > 1:
                ready = multiply([k - 1, 1 - k])
        upper = lax.ppermute(downs[far - 1][: height // 2], "fs", right)
        lower = lax.ppermute(downs[1 - far][height // 2 :], "fs", left)
        downs[far] = jnp.concatenate([upper, lower], axis=0)
        multiply([far - 1, 1 - far])
        multiply([0, far])

        kept = [None] * per_chip
        order = sorted(range(per_chip), key=lambda g: max(
            min(h, n_fs - h) for h in range(g, n_fs, per_chip)
        ))
        for g in order:
            members = list(range(g, n_fs, per_chip))
            owners = [shard_at(here - h) // per_chip for h in members]

            def block_of(target):
                block = partials[members[-1]]
                for h, owner in zip(members[:-1], owners[:-1]):
                    block = jnp.where(owner == target, partials[h], block)
                return block

            total = block_of(chip).astype(jnp.float32)
            for shift in range(1, chips):
                pairs = [(t, (t + 2 * shift) % n_tp) for t in range(n_tp)]
                sent = block_of((chip + shift) % chips)
                total = total + lax.ppermute(sent, "tp", pairs).astype(jnp.float32)
            kept[g] = total
        squares = sum(jnp.sum(jnp.square(kept[g]), axis=1) for g in order)
        squares = lax.psum(squares, "tp")

        whole = jnp.stack([x.astype(jnp.bfloat16) for x in kept])
        half = per_chip // 2

        def columns_of(core_index):
            found = []
            for s in range(half):
                j = chip * per_chip + core_index * half + s
                group = (here - place_of(j)) % per_chip
                found.append(lax.dynamic_index_in_dim(whole, group, keepdims=False))
            return jnp.concatenate(found, axis=1)

        ours = columns_of(core)
        theirs = lax.ppermute(columns_of(1 - core), "tp", sibling)
        parts = []
        for s in range(half):
            a = ours[:, s * side : (s + 1) * side]
            b = theirs[:, s * side : (s + 1) * side]
            parts += [jnp.where(core == 0, a, b), jnp.where(core == 0, b, a)]
        own_columns = jnp.concatenate(parts, axis=1).astype(jnp.float32)
        mean_square = squares / (out_gain.shape[0] * n_tp)
        scaled = own_columns * lax.rsqrt(mean_square + EPSILON)[:, None] * out_gain[None, :]
        return scaled.astype(jnp.bfloat16)

    return body


def solution(mesh):
    return jax.shard_map(
        make_body(mesh.shape["fs"], mesh.shape["tp"]),
        mesh=mesh,
        in_specs=(P("fs", None), P(), P("fs", "tp"), P("fs", "tp"), P("tp", "fs"), P("tp")),
        out_specs=P("fs", "tp"),
        check_vma=False,
    )
```
